32 devices in a mesh: ep: 8 (over z, x), tp: 4 (over y, core).
Axes of the slice: x: 2, y: 2, z: 4, core: 2. Of those that a mesh axis runs over, the one named last changes fastest.
Arguments:
- mix_input: bfloat16 [1024, 2048], P('ep'), may hold values from -6 to 6
- mix_gain: float32 [2048], replicated, may hold values from 0.1 to 1.9
- pool_in_weight: bfloat16 [2048, 1024], P(None, 'tp'), may hold values from -0.125 to 0.125
- pool_out_weight: bfloat16 [1024, 2048], P(None, 'tp'), may hold values from -0.1875 to 0.1875
- moe_input: bfloat16 [1536, 2048], P('ep'), may hold values from -6 to 6
- moe_gain: float32 [2048], replicated, may hold values from 0.1 to 1.9
- group_router: bfloat16 [2048, 4], replicated, may hold values from -0.125 to 0.125
- expert_router: bfloat16 [2048, 8], replicated, may hold values from -0.125 to 0.125
- routes: int32 [1536, 2], P('ep'), may hold values from 0 to 7, as said below
- expert_gate: bfloat16 [8, 2048, 4096], P('ep', None, 'tp'), may hold values from -0.125 to 0.125
- expert_up: bfloat16 [8, 2048, 4096], P('ep', None, 'tp'), may hold values from -0.125 to 0.125
- expert_down: bfloat16 [8, 4096, 2048], P('ep', 'tp'), may hold values from -0.375 to 0.375
Outputs:
- mixed: bfloat16 [1024, 2048], P('ep', 'tp')
- experts_out: bfloat16 [1536, 2048], P('ep', 'tp')
The draws below stay inside these ranges and needn't reach their ends.
Inputs may be any that keep to these rules, and one draw needn't show every extreme that they name: `routes`: each row names two different experts of one group: the 2 experts numbered k * 2 to k * 2 + 1 for a group k. Among the rows of one device no expert is named more than 96 times, and in the rows of every device some expert is named exactly 96 times.
All inputs are finite; a program needn't handle non-finite values.
Results may differ from the reference program's by a relative error of at most 0.019.
Values may be sent and summed in bfloat16 or wider, within the bound.
A program may use at most 64 MiB of HBM per device.

```python
import jax
import jax.numpy as jnp
from jax import lax

D = 2048
P_SIZE = 1024
FFE = 4096
GROUPS = 4
EXPERTS = 8
EPG = 2
ROWS = 192
CAP = 96
TOK_MOE = 1536
TOK_MIX = 1024
N_TP = 4


def draw_routes(key, part):
    hot_rows = 2 * ROWS // GROUPS

    def one_block(block_key):
        keys = jax.random.split(block_key, 4)
        hot_group = jax.random.randint(keys[0], (), 0, GROUPS)
        shifts = jax.random.randint(keys[1], (GROUPS,), 0, EPG - 1)
        offsets = jax.random.randint(keys[2], (GROUPS,), 0, EPG)
        order_rank = jnp.arange(ROWS, dtype=jnp.int32)
        beyond = jnp.maximum(order_rank - hot_rows, 0)
        is_hot = order_rank < hot_rows
        group_of = jnp.where(is_hot, hot_group, (hot_group + 1 + beyond % (GROUPS - 1)) % GROUPS)
        within = jnp.where(is_hot, order_rank, beyond // (GROUPS - 1))
        first_pick = (within + offsets[group_of]) % EPG
        second_pick = (first_pick + 1 + shifts[group_of]) % EPG
        pairs = jnp.stack([group_of * EPG + first_pick, group_of * EPG + second_pick], axis=1)
        shuffle = jax.random.permutation(keys[3], ROWS)
        return pairs[jnp.argsort(shuffle)]
    block_keys = jax.random.split(jax.random.fold_in(key, 7), TOK_MOE // ROWS)
    return jax.vmap(one_block)(block_keys).reshape(TOK_MOE, 2).astype(jnp.int32)


def block_levels(rng, dims, shards, smallest, largest):
    loudness = 1.0
    for dim, shards_of in shards:
        steps = jax.random.uniform(jax.random.fold_in(jax.random.fold_in(rng, 6), dim), (shards_of,), jnp.float32, smallest / len(shards), largest / len(shards))
        loudness = loudness * jnp.repeat(jnp.exp(steps), dims[dim] // shards_of).reshape((-1,) + (1,) * (len(dims) - 1 - dim))
    return loudness


def gaussian(stream_key, shape, spread, reach, cuts=(), kind=jnp.bfloat16):
    result = spread * jax.random.normal(stream_key, shape, jnp.float32)
    if cuts:
        result = result * block_levels(stream_key, shape, cuts, -0.22, 0.18)
    return jnp.clip(result, -reach, reach).astype(kind)


def setup_inputs(seed: int = 0) -> dict:
    seeds = jax.random.split(jax.random.key(seed), 13)
    mix_input = gaussian(seeds[0], (TOK_MIX, D), 1.0, 6.0, ((0, 8),))
    mix_gain = jnp.clip(1.0 + 0.18 * jax.random.normal(seeds[1], (D,), jnp.float32), 0.1, 1.9)
    pool_in_weight = gaussian(seeds[2], (D, P_SIZE), D ** -0.5, 0.125, ((1, 4),))
    pool_out_weight = gaussian(seeds[3], (P_SIZE, D), P_SIZE ** -0.5, 0.1875, ((1, 4),))
    moe_input = gaussian(seeds[4], (TOK_MOE, D), 1.0, 6.0, ((0, 8),))
    moe_gain = jnp.clip(1.0 + 0.18 * jax.random.normal(seeds[5], (D,), jnp.float32), 0.1, 1.9)
    group_router = gaussian(seeds[6], (D, GROUPS), D ** -0.5, 0.125)
    expert_router = gaussian(seeds[7], (D, EXPERTS), D ** -0.5, 0.125)
    routes = draw_routes(jax.random.fold_in(seeds[12], 71), 0)
    expert_gate = gaussian(seeds[9], (EXPERTS, D, FFE), D ** -0.5, 0.125, ((0, 8), (2, 4)))
    expert_up = gaussian(seeds[10], (EXPERTS, D, FFE), D ** -0.5, 0.125, ((0, 8), (2, 4)))
    expert_down = gaussian(seeds[11], (EXPERTS, FFE, D), (FFE // 16) ** -0.5, 0.375, ((0, 8), (1, 4)))
    return dict(mix_input=mix_input, mix_gain=mix_gain, pool_in_weight=pool_in_weight, pool_out_weight=pool_out_weight, moe_input=moe_input, moe_gain=moe_gain, group_router=group_router, expert_router=expert_router, routes=routes, expert_gate=expert_gate, expert_up=expert_up, expert_down=expert_down)


epsilon = 1e-06

def normalize(row_data, gain_vector):
    values = row_data.astype(jnp.float32)
    inverse_rms = lax.rsqrt(lax.optimization_barrier(jnp.mean(values * values, axis=-1, keepdims=True)) + epsilon)
    return (values * inverse_rms * gain_vector).astype(jnp.bfloat16)

def pool_channels(pool_input):
    length = pool_input.shape[0]
    values = pool_input.astype(jnp.float32)
    totals = jnp.concatenate([jnp.zeros((1, values.shape[1]), jnp.float32), jnp.cumsum(values, axis=0)], axis=0)
    group_width = values.shape[1] // 4
    places = jnp.arange(length, dtype=jnp.int32)
    pieces = []
    for group_index in range(4):
        half_span = 2 ** group_index
        lower_end = jnp.maximum(places - half_span, 0)
        upper_end = jnp.minimum(places + half_span, length)
        channel_block = totals[:, group_index * group_width:(group_index + 1) * group_width]
        counts = (upper_end - lower_end).astype(jnp.float32)
        window_mean = (channel_block[upper_end] - channel_block[lower_end]) / counts[:, None]
        pieces.append(window_mean - values[:, group_index * group_width:(group_index + 1) * group_width])
    return jnp.concatenate(pieces, axis=1).astype(jnp.bfloat16)

def routing(normed, group_router, expert_router, routes):
    group_logits = jnp.dot(normed, group_router, preferred_element_type=jnp.float32)
    expert_logits = jnp.dot(normed, expert_router, preferred_element_type=jnp.float32)
    group_count = group_router.shape[1]
    expert_count = expert_router.shape[1]
    per_group = expert_count // group_count
    first_id = routes[:, 0]
    second_id = routes[:, 1]
    chosen_group = first_id // per_group
    group_match = jnp.arange(group_count, dtype=jnp.int32)[None, :] == chosen_group[:, None]
    chosen_logit = lax.optimization_barrier(jnp.sum(jnp.where(group_match, group_logits, 0.0), axis=1))
    group_share = 1.0 / lax.optimization_barrier(jnp.sum(jnp.exp(group_logits - chosen_logit[:, None]), axis=1))
    expert_ids = jnp.arange(expert_count, dtype=jnp.int32)[None, :]
    first_logit = lax.optimization_barrier(jnp.sum(jnp.where(expert_ids == first_id[:, None], expert_logits, 0.0), axis=1))
    second_logit = lax.optimization_barrier(jnp.sum(jnp.where(expert_ids == second_id[:, None], expert_logits, 0.0), axis=1))
    first_weight = group_share * jax.nn.sigmoid(first_logit - second_logit)
    second_weight = group_share * jax.nn.sigmoid(second_logit - first_logit)
    return (first_weight, second_weight)

def reference(mix_input, mix_gain, pool_in_weight, pool_out_weight, moe_input, moe_gain, group_router, expert_router, routes, expert_gate, expert_up, expert_down):
    normed_mix = normalize(mix_input, mix_gain)
    pool_input = jnp.dot(normed_mix, pool_in_weight, preferred_element_type=jnp.float32).astype(jnp.bfloat16)
    pooled = pool_channels(pool_input)
    mixed = jnp.dot(pooled, pool_out_weight, preferred_element_type=jnp.float32).astype(jnp.bfloat16)
    normed_moe = normalize(moe_input, moe_gain)
    first_weight, second_weight = routing(normed_moe, group_router, expert_router, routes)
    tokens = normed_moe.shape[0]
    features = normed_moe.shape[1]
    expert_count = expert_router.shape[1]
    blocks = tokens // ROWS
    copy_weights = jnp.stack([first_weight, second_weight], axis=1).reshape(-1)
    block_ids = routes.reshape(blocks, 2 * ROWS)
    onehot = (block_ids[:, :, None] == jnp.arange(expert_count, dtype=jnp.int32)[None, None, :]).astype(jnp.int32)
    before = jnp.cumsum(onehot, axis=1) - onehot
    slot_rank = jnp.take_along_axis(before, block_ids[:, :, None], axis=2)[:, :, 0]
    slot_place = jnp.arange(blocks, dtype=jnp.int32)[:, None] * CAP + slot_rank
    copy_index = jnp.arange(2 * tokens, dtype=jnp.int32).reshape(blocks, 2 * ROWS)
    slot_table = jnp.full((expert_count, blocks * CAP), 2 * tokens, jnp.int32)
    slot_table = slot_table.at[block_ids.reshape(-1), slot_place.reshape(-1)].set(copy_index.reshape(-1))
    padded_rows = jnp.concatenate([normed_moe, jnp.zeros((1, features), jnp.bfloat16)], axis=0)
    padded_weights = jnp.concatenate([copy_weights, jnp.zeros((1,), jnp.float32)], axis=0)
    hidden_block = FFE // N_TP

    def one_expert(running, inputs):
        slot_copies, gate_matrix, up_matrix, down_matrix = inputs
        token_index = slot_copies // 2
        rows_in = padded_rows[token_index]
        gate_values = jnp.dot(rows_in, gate_matrix, preferred_element_type=jnp.float32)
        up_values = jnp.dot(rows_in, up_matrix, preferred_element_type=jnp.float32)
        hidden = (jax.nn.silu(gate_values) * up_values).astype(jnp.bfloat16)
        block_parts = jnp.einsum('sjf,jfd->jsd', hidden.reshape(-1, N_TP, hidden_block).astype(jnp.float32), down_matrix.reshape(N_TP, hidden_block, features).astype(jnp.float32))
        rounded_parts = lax.optimization_barrier(block_parts.astype(jnp.bfloat16))
        answer = lax.optimization_barrier(jnp.sum(rounded_parts.astype(jnp.float32), axis=0)).astype(jnp.bfloat16)
        contribution = padded_weights[slot_copies][:, None] * answer.astype(jnp.float32)
        return (running.at[token_index].add(contribution), None)
    start_sum = jnp.zeros((tokens + 1, features), jnp.float32)
    running, _ = lax.scan(one_expert, start_sum, (slot_table, expert_gate, expert_up, expert_down))
    experts_out = running[:tokens].astype(jnp.bfloat16)
    return (mixed, experts_out)
```

```python
import functools

import jax
import jax.numpy as jnp
from jax import lax
from jax.experimental import pallas as pl
from jax.experimental.pallas import tpu as pltpu
from jax.sharding import PartitionSpec as P

MESH = pl.DeviceIdType.MESH
EPSILON = 1e-06
HALO = 16
F32 = jnp.float32
BF16 = jnp.bfloat16


def tile_of(width, most):
    return most if width % most == 0 else width


def block_kernel(
    sizes,
    og_ref, pool_ref, ids_ref, weights_ref, wg_hbm, wu_hbm, wd_hbm, pw_hbm,
    mixed_ref, out_ref,
    wg, wu, wd, pw, rx, hid, part, core_in, y_in, answer, back, ext, pooled_all,
    w_sem, own_sem, d_send, d_recv, ay_send, ay_recv, ac_send, ac_recv,
    rc_send, rc_recv, ry_send, ry_recv, b_send, b_recv, h_send, h_recv, p_send, p_recv,
):
    E, T, steps, per_group = sizes
    Y = T // 2
    each = E // steps
    R, D = og_ref.shape[1], og_ref.shape[2]
    F, H = D // T, wg.shape[1]
    rows = each * R
    me, t = lax.axis_index("ep"), lax.axis_index("tp")
    y, c = t // 2, t % 2
    mate = t + 1 - 2 * c

    def ep_of(shift):
        return lax.rem(me + shift + E, E)

    def y_of(shift):
        return lax.rem(y + shift + Y, Y)

    def cols(index):
        return pl.ds(pl.multiple_of(index * F, F), F)

    def remote(src, dst, send, recv, where):
        return pltpu.make_async_remote_copy(
            src_ref=src, dst_ref=dst, send_sem=send, recv_sem=recv,
            device_id=where, device_id_type=MESH,
        )

    loads = [
        pltpu.make_async_copy(src, dst, w_sem.at[i])
        for i, (src, dst) in enumerate(((wg_hbm, wg), (wu_hbm, wu), (wd_hbm, wd), (pw_hbm, pw)))
    ]
    own = pltpu.make_async_copy(og_ref.at[me // per_group], rx.at[pl.ds(0, R)], own_sem)
    own.start()

    barrier = pltpu.get_barrier_semaphore()
    for d in range(1, E):
        pl.semaphore_signal(barrier, inc=1, device_id=(ep_of(d), t), device_id_type=MESH)
    for j in range(1, T):
        pl.semaphore_signal(
            barrier, inc=1, device_id=(me, lax.rem(t + j, T)), device_id_type=MESH
        )
    pl.semaphore_wait(barrier, E - 1 + T - 1)

    dispatch = {}
    for d in range(1, E):
        dest = ep_of(d)
        dispatch[d] = remote(
            og_ref.at[dest // per_group, :, cols(t)], rx.at[pl.ds(d * R, R), cols(t)],
            d_send.at[d], d_recv.at[d], (dest, t),
        )
        dispatch[d].start()
    n = pool_ref.shape[0]
    halo = [
        remote(pool_ref.at[pl.ds(n - HALO, HALO)], ext.at[pl.ds(0, HALO)],
               h_send.at[0], h_recv.at[0], (ep_of(1), t)),
        remote(pool_ref.at[pl.ds(0, HALO)], ext.at[pl.ds(n + HALO, HALO)],
               h_send.at[1], h_recv.at[1], (ep_of(-1), t)),
    ]
    for copy in halo:
        copy.start()
    for copy in loads:
        copy.start()

    gather_y, gather_c, give_c, give_y, answers = {}, {}, {}, {}, {}

    def span(g):
        first = g * rows + (R if g == 0 else 0)
        return pl.ds(first, (g + 1) * rows - first)

    def to_mate(g, j):
        place = rx.at[span(g), cols(2 * y_of(-j) + c)]
        gather_c[g, j] = remote(place, place, ac_send.at[g, j], ac_recv.at[g, j], (me, mate))
        gather_c[g, j].start()

    def arrive(g):
        for d in range(max(1, g * each), (g + 1) * each):
            dispatch[d].wait_recv()
        place = rx.at[span(g), cols(t)]
        for j in range(1, Y):
            gather_y[g, j] = remote(
                place, place, ay_send.at[g, j], ay_recv.at[g, j], (me, 2 * y_of(j) + c)
            )
            gather_y[g, j].start()
        to_mate(g, 0)

    def forward(g):
        for j in range(1, Y):
            gather_y[g, j].wait_recv()
            to_mate(g, j)

    def compute(g):
        for j in range(Y):
            gather_c[g, j].wait_recv()
        if g == 0:
            own.wait()
            loads[0].wait()
            loads[1].wait()
        block = pl.ds(g * rows, rows)
        width = tile_of(H, 256)

        @pl.loop(0, H // width)
        def _(i):
            at = pl.ds(pl.multiple_of(i * width, width), width)
            x = rx[block, :]
            gate = jnp.dot(x, wg[:, at], preferred_element_type=F32)
            up = jnp.dot(x, wu[:, at], preferred_element_type=F32)
            hid[:, at] = (gate / (1.0 + jnp.exp(-gate)) * up).astype(BF16)

        if g == 0:
            loads[2].wait()
        wide = tile_of(D, 512)

        @pl.loop(0, D // wide)
        def _(i):
            at = pl.ds(pl.multiple_of(i * wide, wide), wide)
            part[block, at] = jnp.dot(
                hid[...], wd[:, at], preferred_element_type=F32
            ).astype(BF16)

        for j in reversed(range(Y)):
            give_c[g, j] = remote(
                part.at[block, cols(2 * y_of(j) + 1 - c)], core_in.at[g, j],
                rc_send.at[g, j], rc_recv.at[g, j], (me, mate),
            )
            give_c[g, j].start()

    def reduce_core(g):
        block = pl.ds(g * rows, rows)
        for j in reversed(range(Y)):
            give_c[g, j].wait_recv()
            mine = part[block, cols(2 * y_of(j) + c)]
            core_in[g, j] = (core_in[g, j].astype(F32) + mine.astype(F32)).astype(BF16)
            if j:
                give_y[g, j] = remote(
                    core_in.at[g, j], y_in.at[g, j], ry_send.at[g, j], ry_recv.at[g, j],
                    (me, 2 * y_of(j) + c),
                )
                give_y[g, j].start()

    def reduce_y(g):
        total = core_in[g, 0].astype(F32)
        for j in range(1, Y):
            give_y[g, j].wait_recv()
            total += y_in[g, j].astype(F32)
        answer[pl.ds(g * rows, rows), :] = total.astype(BF16)
        for d in range(max(1, g * each), (g + 1) * each):
            answers[d] = remote(
                answer.at[pl.ds(d * R, R)], back.at[d], b_send.at[d], b_recv.at[d],
                (ep_of(-d), t),
            )
            answers[d].start()

    def pool():
        ext[pl.ds(HALO, n), :] = pool_ref[...]
        for copy in halo:
            copy.wait_recv()
        length = n * E
        channels = pool_ref.shape[1]
        half = jnp.left_shift(jnp.int32(1), t * channels // (channels * T // 4))
        at = me * n + lax.broadcasted_iota(jnp.int32, (n, n + 2 * HALO), 0)
        source = me * n - HALO + lax.broadcasted_iota(jnp.int32, (n, n + 2 * HALO), 1)
        low, high = jnp.maximum(at - half, 0), jnp.minimum(at + half, length)
        band = jnp.where((source >= low) & (source < high), 1.0, 0.0).astype(BF16)
        sums = jnp.dot(band, ext[...], preferred_element_type=F32)
        row = me * n + lax.broadcasted_iota(jnp.int32, (n, 1), 0)
        count = (jnp.minimum(row + half, length) - jnp.maximum(row - half, 0)).astype(F32)
        pooled_all[0] = (sums / count - pool_ref[...].astype(F32)).astype(BF16)
        sent = []
        for j in range(1, T):
            sent.append(remote(
                pooled_all.at[0], pooled_all.at[j], p_send.at[j], p_recv.at[j],
                (me, lax.rem(t + j, T)),
            ))
            sent[-1].start()
        return sent

    def mix(sent):
        loads[3].wait()
        total = jnp.dot(pooled_all[0], pw[t], preferred_element_type=F32)
        for j in range(1, T):
            sent[j - 1].wait_recv()
            total += jnp.dot(
                pooled_all[j], pw[lax.rem(t + T - j, T)], preferred_element_type=F32
            )
        mixed_ref[...] = total.astype(BF16)

    sent = pool()
    stages = (arrive, forward, compute, reduce_core, reduce_y)
    lead = (0, 1, 2, 3, 4)
    for beat in range(steps + lead[-1]):
        for stage, late in zip(stages, lead):
            if 0 <= beat - late < steps:
                stage(beat - late)
        if beat == 1:
            mix(sent)

    slot = ids_ref[:, 0:1]
    first, second = ids_ref[:, 1:2], ids_ref[:, 2:3]
    first_weight, second_weight = weights_ref[:, 0:1], weights_ref[:, 1:2]
    local = ids_ref.shape[0]
    place = lax.broadcasted_iota(jnp.int32, (local, R), 1)
    total = jnp.zeros((local, F), F32)
    for d in range(E):
        expert = ep_of(d)
        weight = jnp.where(first == expert, first_weight, jnp.where(second == expert, second_weight, 0.0))
        pick = jnp.where(slot == place + expert // per_group * R, weight, 0.0)
        high = pick.astype(BF16)
        low = (pick - high.astype(F32)).astype(BF16)
        if d == 0:
            rows_back = answer[pl.ds(0, R), :]
        else:
            answers[d].wait_recv()
            rows_back = back[d]
        total += jnp.dot(high, rows_back, preferred_element_type=F32)
        total += jnp.dot(low, rows_back, preferred_element_type=F32)
    out_ref[...] = total.astype(BF16)

    for group in (dispatch, gather_y, gather_c, give_c, give_y, answers):
        for copy in group.values():
            copy.wait_send()
    for copy in halo + sent:
        copy.wait_send()


def normalize(row_data, gain_vector):
    values = row_data.astype(F32)
    inverse_rms = lax.rsqrt(jnp.mean(values * values, axis=-1, keepdims=True) + EPSILON)
    return (values * inverse_rms * gain_vector).astype(BF16)


def on_device(
    mix_input, mix_gain, pool_in_weight, pool_out_weight, moe_input, moe_gain,
    group_router, expert_router, routes, expert_gate, expert_up, expert_down,
):
    E, T = lax.axis_size("ep"), lax.axis_size("tp")
    normed_moe = normalize(moe_input, moe_gain)
    local, D = normed_moe.shape
    groups, experts = group_router.shape[1], expert_router.shape[1]
    per_group = experts // groups
    R = 2 * local // groups
    chosen = routes[:, 0] // per_group
    match = jnp.arange(groups, dtype=jnp.int32)[None, :] == chosen[:, None]
    places = jnp.arange(local, dtype=jnp.int32)
    before = (places[None, :] < places[:, None]) & (chosen[None, :] == chosen[:, None])
    rank = jnp.sum(before.astype(jnp.int32), axis=1)
    slot = chosen * R + rank
    select = (jnp.arange(groups * R, dtype=jnp.int32)[:, None] == slot[None, :]).astype(BF16)
    outgoing = jnp.dot(select, normed_moe, preferred_element_type=F32).astype(BF16)
    outgoing = outgoing.reshape(groups, R, D)

    logits = jnp.dot(
        normed_moe, jnp.concatenate([group_router, expert_router], axis=1),
        preferred_element_type=F32,
    )
    group_logits, expert_logits = logits[:, :groups], logits[:, groups:]
    chosen_logit = jnp.sum(jnp.where(match, group_logits, 0.0), axis=1)
    share = 1.0 / jnp.sum(jnp.exp(group_logits - chosen_logit[:, None]), axis=1)
    expert_ids = jnp.arange(experts, dtype=jnp.int32)[None, :]
    first_logit = jnp.sum(jnp.where(expert_ids == routes[:, 0:1], expert_logits, 0.0), axis=1)
    second_logit = jnp.sum(jnp.where(expert_ids == routes[:, 1:2], expert_logits, 0.0), axis=1)
    weights = jnp.stack(
        [share * jax.nn.sigmoid(first_logit - second_logit),
         share * jax.nn.sigmoid(second_logit - first_logit)], axis=1)
    ids = jnp.concatenate([slot[:, None], routes], axis=1)

    pool_input = jnp.dot(
        normalize(mix_input, mix_gain), pool_in_weight, preferred_element_type=F32
    ).astype(BF16)

    n, channels = pool_input.shape
    F, H, Y = D // T, expert_gate.shape[2], T // 2
    F2 = pool_out_weight.shape[1]
    steps = 4
    rows = E // steps * R
    dma = pltpu.SemaphoreType.DMA
    vmem = pl.BlockSpec(memory_space=pltpu.VMEM)
    hbm = pl.BlockSpec(memory_space=pl.ANY)
    return pl.pallas_call(
        functools.partial(block_kernel, (E, T, steps, per_group)),
        out_shape=(
            jax.ShapeDtypeStruct((n, F2), BF16),
            jax.ShapeDtypeStruct((local, F), BF16),
        ),
        in_specs=[vmem] * 4 + [hbm] * 4,
        out_specs=(vmem, vmem),
        scratch_shapes=[
            pltpu.VMEM((D, H), BF16),
            pltpu.VMEM((D, H), BF16),
            pltpu.VMEM((H, D), BF16),
            pltpu.VMEM((T, channels, F2), BF16),
            pltpu.VMEM((E * R, D), BF16),
            pltpu.VMEM((rows, H), BF16),
            pltpu.VMEM((E * R, D), BF16),
            pltpu.VMEM((steps, Y, rows, F), BF16),
            pltpu.VMEM((steps, Y, rows, F), BF16),
            pltpu.VMEM((E * R, F), BF16),
            pltpu.VMEM((E, R, F), BF16),
            pltpu.VMEM((n + 2 * HALO, channels), BF16),
            pltpu.VMEM((T, n, channels), BF16),
            dma((4,)), dma, dma((E,)), dma((E,)),
            dma((steps, Y)), dma((steps, Y)), dma((steps, Y)), dma((steps, Y)),
            dma((steps, Y)), dma((steps, Y)), dma((steps, Y)), dma((steps, Y)),
            dma((E,)), dma((E,)), dma((2,)), dma((2,)), dma((T,)), dma((T,)),
        ],
        compiler_params=pltpu.CompilerParams(
            collective_id=0, has_side_effects=True, vmem_limit_bytes=60 * 1024 * 1024
        ),
    )(
        outgoing, pool_input, ids, weights,
        expert_gate.reshape(D, H), expert_up.reshape(D, H), expert_down.reshape(H, D),
        pool_out_weight.reshape(T, channels, F2),
    )


def solution(mesh):
    in_specs = (
        P("ep", None), P(), P(None, "tp"), P(None, "tp"), P("ep", None), P(), P(), P(),
        P("ep", None), P("ep", None, "tp"), P("ep", None, "tp"), P("ep", "tp", None),
    )
    return jax.shard_map(
        on_device, mesh=mesh, in_specs=in_specs, out_specs=(P("ep", "tp"), P("ep", "tp")),
        check_vma=False,
    )
```

```python
import functools

import jax
import jax.numpy as jnp
from jax import lax
from jax.experimental import pallas as pl
from jax.experimental.pallas import tpu as pltpu
from jax.sharding import PartitionSpec as P

MESH = pl.DeviceIdType.MESH
EPSILON = 1e-06
HALO = 16
F32 = jnp.float32
BF16 = jnp.bfloat16


def tile_of(width, most):
    return most if width % most == 0 else width


def normalize(rows_ref, gain_ref, result):
    count = 32 if rows_ref.shape[0] % 32 == 0 else rows_ref.shape[0]

    @pl.loop(0, rows_ref.shape[0] // count)
    def _(i):
        at = pl.ds(pl.multiple_of(i * count, count), count)
        values = rows_ref[at, :].astype(F32)
        inverse_rms = lax.rsqrt(jnp.mean(values * values, axis=-1, keepdims=True) + EPSILON)
        result[at, :] = (values * inverse_rms * gain_ref[...]).astype(BF16)


def block_kernel(
    sizes,
    mix_ref, mix_gain_ref, pool_in_ref, moe_ref, moe_gain_ref, router_ref, routes_ref, wg_hbm, wu_hbm, wd_hbm, pw_hbm,
    mixed_ref, out_ref,
    og, normed, normed_mix, pool_ref, wg, wu, wd, pw, rx, hid, part, core_in, y_in, answer, back, ext, pooled_all,
    w_sem, own_sem, d_send, d_recv, ay_send, ay_recv, ac_send, ac_recv,
    rc_send, rc_recv, ry_send, ry_recv, b_send, b_recv, h_send, h_recv, p_send, p_recv,
):
    E, T, steps, per_group = sizes
    Y = T // 2
    each = E // steps
    local, D = moe_ref.shape
    groups = E // per_group
    R = 2 * local // groups
    F, H = D // T, wg.shape[1]
    rows = each * R
    me, t = lax.axis_index("ep"), lax.axis_index("tp")
    y, c = t // 2, t % 2
    mate = t + 1 - 2 * c

    def ep_of(shift):
        return lax.rem(me + shift + E, E)

    def y_of(shift):
        return lax.rem(y + shift + Y, Y)

    def cols(index):
        return pl.ds(pl.multiple_of(index * F, F), F)

    def remote(src, dst, send, recv, where):
        return pltpu.make_async_remote_copy(
            src_ref=src, dst_ref=dst, send_sem=send, recv_sem=recv,
            device_id=where, device_id_type=MESH,
        )

    loads = [
        pltpu.make_async_copy(src, dst, w_sem.at[i])
        for i, (src, dst) in enumerate(((wg_hbm, wg), (wu_hbm, wu), (wd_hbm, wd), (pw_hbm, pw)))
    ]
    for copy in loads:
        copy.start()

    barrier = pltpu.get_barrier_semaphore()
    for d in range(1, E):
        pl.semaphore_signal(barrier, inc=1, device_id=(ep_of(d), t), device_id_type=MESH)
    for j in range(1, T):
        pl.semaphore_signal(
            barrier, inc=1, device_id=(me, lax.rem(t + j, T)), device_id_type=MESH
        )

    normalize(mix_ref, mix_gain_ref, normed_mix)
    pool_ref[...] = jnp.dot(normed_mix[...], pool_in_ref[...], preferred_element_type=F32).astype(BF16)
    normalize(moe_ref, moe_gain_ref, normed)
    first, second = routes_ref[:, 0:1], routes_ref[:, 1:2]

    def lanes(width):
        return lax.broadcasted_iota(jnp.int32, (local, width), 1)

    lane = lanes(128)
    low = lane * per_group
    match = (first >= low) & (first < low + per_group) & (lane < groups)
    before = lax.broadcasted_iota(jnp.int32, (local, local), 0) > lanes(local)
    rank = jnp.dot(
        jnp.where(before, 1.0, 0.0).astype(BF16), jnp.where(match, 1.0, 0.0).astype(BF16),
        preferred_element_type=F32,
    )
    slot = jnp.sum(
        jnp.where(match, rank + (lane * R).astype(F32), 0.0), axis=1, keepdims=True
    ).astype(jnp.int32)
    select = jnp.where(lanes(groups * R) == slot, 1.0, 0.0).astype(BF16)
    piece = tile_of(D, 512)

    @pl.loop(0, D // piece)
    def _(i):
        at = pl.ds(pl.multiple_of(i * piece, piece), piece)
        og[:, at] = lax.dot_general(
            select, normed[:, at], (((0,), (0,)), ((), ())), preferred_element_type=F32
        ).astype(BF16)

    pl.semaphore_wait(barrier, E - 1 + T - 1)

    def group_rows(expert):
        return pl.ds(pl.multiple_of(expert // per_group * R, R), R)

    own = pltpu.make_async_copy(og.at[group_rows(me)], rx.at[pl.ds(0, R)], own_sem)
    own.start()

    n = pool_ref.shape[0]
    halo = [
        remote(pool_ref.at[pl.ds(n - HALO, HALO)], ext.at[pl.ds(0, HALO)],
               h_send.at[0], h_recv.at[0], (ep_of(1), t)),
        remote(pool_ref.at[pl.ds(0, HALO)], ext.at[pl.ds(n + HALO, HALO)],
               h_send.at[1], h_recv.at[1], (ep_of(-1), t)),
    ]
    for copy in halo:
        copy.start()
    dispatch = {}
    for d in range(1, E):
        dest = ep_of(d)
        part_of = cols(t)
        dispatch[d] = remote(
            og.at[group_rows(dest), part_of], rx.at[pl.ds(d * R, R), part_of],
            d_send.at[d], d_recv.at[d], (dest, t),
        )
        dispatch[d].start()

    gather_y, gather_c, give_c, give_y, answers = {}, {}, {}, {}, {}

    def span(g):
        first = g * rows + (R if g == 0 else 0)
        return pl.ds(first, (g + 1) * rows - first)

    def to_mate(g, j):
        place = rx.at[span(g), cols(2 * y_of(-j) + c)]
        gather_c[g, j] = remote(place, place, ac_send.at[g, j], ac_recv.at[g, j], (me, mate))
        gather_c[g, j].start()

    def arrive(g):
        for d in range(max(1, g * each), (g + 1) * each):
            dispatch[d].wait_recv()
        place = rx.at[span(g), cols(t)]
        for j in range(1, Y):
            gather_y[g, j] = remote(
                place, place, ay_send.at[g, j], ay_recv.at[g, j], (me, 2 * y_of(j) + c)
            )
            gather_y[g, j].start()
        to_mate(g, 0)

    def forward(g):
        for j in range(1, Y):
            gather_y[g, j].wait_recv()
            to_mate(g, j)

    def compute(g):
        for j in range(Y):
            gather_c[g, j].wait_recv()
        if g == 0:
            own.wait()
            loads[0].wait()
            loads[1].wait()
        block = pl.ds(g * rows, rows)
        width = tile_of(H, 256)

        @pl.loop(0, H // width)
        def _(i):
            at = pl.ds(pl.multiple_of(i * width, width), width)
            x = rx[block, :]
            gate = jnp.dot(x, wg[:, at], preferred_element_type=F32)
            up = jnp.dot(x, wu[:, at], preferred_element_type=F32)
            hid[:, at] = (gate / (1.0 + jnp.exp(-gate)) * up).astype(BF16)

        if g == 0:
            loads[2].wait()
        wide = tile_of(D, 512)

        @pl.loop(0, D // wide)
        def _(i):
            at = pl.ds(pl.multiple_of(i * wide, wide), wide)
            part[block, at] = jnp.dot(
                hid[...], wd[:, at], preferred_element_type=F32
            ).astype(BF16)

        for j in reversed(range(Y)):
            give_c[g, j] = remote(
                part.at[block, cols(2 * y_of(j) + 1 - c)], core_in.at[g, j],
                rc_send.at[g, j], rc_recv.at[g, j], (me, mate),
            )
            give_c[g, j].start()

    def reduce_core(g):
        block = pl.ds(g * rows, rows)
        for j in reversed(range(Y)):
            give_c[g, j].wait_recv()
            mine = part[block, cols(2 * y_of(j) + c)]
            core_in[g, j] = (core_in[g, j].astype(F32) + mine.astype(F32)).astype(BF16)
            if j:
                give_y[g, j] = remote(
                    core_in.at[g, j], y_in.at[g, j], ry_send.at[g, j], ry_recv.at[g, j],
                    (me, 2 * y_of(j) + c),
                )
                give_y[g, j].start()

    def reduce_y(g):
        total = core_in[g, 0].astype(F32)
        for j in range(1, Y):
            give_y[g, j].wait_recv()
            total += y_in[g, j].astype(F32)
        answer[pl.ds(g * rows, rows), :] = total.astype(BF16)
        for d in range(max(1, g * each), (g + 1) * each):
            answers[d] = remote(
                answer.at[pl.ds(d * R, R)], back.at[d], b_send.at[d], b_recv.at[d],
                (ep_of(-d), t),
            )
            answers[d].start()

    def pool():
        ext[pl.ds(HALO, n), :] = pool_ref[...]
        for copy in halo:
            copy.wait_recv()
        length = n * E
        channels = pool_ref.shape[1]
        half = jnp.left_shift(jnp.int32(1), t * channels // (channels * T // 4))
        at = me * n + lax.broadcasted_iota(jnp.int32, (n, n + 2 * HALO), 0)
        source = me * n - HALO + lax.broadcasted_iota(jnp.int32, (n, n + 2 * HALO), 1)
        low, high = jnp.maximum(at - half, 0), jnp.minimum(at + half, length)
        band = jnp.where((source >= low) & (source < high), 1.0, 0.0).astype(BF16)
        sums = jnp.dot(band, ext[...], preferred_element_type=F32)
        row = me * n + lax.broadcasted_iota(jnp.int32, (n, 1), 0)
        count = (jnp.minimum(row + half, length) - jnp.maximum(row - half, 0)).astype(F32)
        pooled_all[0] = (sums / count - pool_ref[...].astype(F32)).astype(BF16)
        sent = []
        for j in range(1, T):
            sent.append(remote(
                pooled_all.at[0], pooled_all.at[j], p_send.at[j], p_recv.at[j],
                (me, lax.rem(t + j, T)),
            ))
            sent[-1].start()
        return sent

    def mix(sent):
        loads[3].wait()
        total = jnp.dot(pooled_all[0], pw[t], preferred_element_type=F32)
        for j in range(1, T):
            sent[j - 1].wait_recv()
            total += jnp.dot(
                pooled_all[j], pw[lax.rem(t + T - j, T)], preferred_element_type=F32
            )
        mixed_ref[...] = total.astype(BF16)

    logits = jnp.dot(normed[...], router_ref[...], preferred_element_type=F32)
    lane = lanes(groups + E)
    low = lane * per_group
    match = (first >= low) & (first < low + per_group) & (lane < groups)

    def logit_at(mask):
        return jnp.sum(jnp.where(mask, logits, 0.0), axis=1, keepdims=True)

    spread = jnp.where(lane < groups, jnp.exp(logits - logit_at(match)), 0.0)
    share = 1.0 / jnp.sum(spread, axis=1, keepdims=True)
    gap = logit_at(lane == first + groups) - logit_at(lane == second + groups)
    first_weight = share / (1.0 + jnp.exp(-gap))
    second_weight = share / (1.0 + jnp.exp(gap))

    sent = pool()
    stages = (arrive, forward, compute, reduce_core, reduce_y)
    lead = (0, 1, 2, 3, 4)
    for beat in range(steps + lead[-1]):
        for stage, late in zip(stages, lead):
            if 0 <= beat - late < steps:
                stage(beat - late)
        if beat == steps + 1:
            mix(sent)

    place = lanes(R)
    total = jnp.zeros((local, F), F32)
    for d in range(E):
        expert = ep_of(d)
        weight = jnp.where(first == expert, first_weight, jnp.where(second == expert, second_weight, 0.0))
        pick = jnp.where(slot == place + expert // per_group * R, weight, 0.0)
        high = pick.astype(BF16)
        low = (pick - high.astype(F32)).astype(BF16)
        if d == 0:
            rows_back = answer[pl.ds(0, R), :]
        else:
            answers[d].wait_recv()
            rows_back = back[d]
        total += jnp.dot(high, rows_back, preferred_element_type=F32)
        total += jnp.dot(low, rows_back, preferred_element_type=F32)
    out_ref[...] = total.astype(BF16)

    for group in (dispatch, gather_y, gather_c, give_c, give_y, answers):
        for copy in group.values():
            copy.wait_send()
    for copy in halo + sent:
        copy.wait_send()


def on_device(
    mix_input, mix_gain, pool_in_weight, pool_out_weight, moe_input, moe_gain,
    group_router, expert_router, routes, expert_gate, expert_up, expert_down,
):
    E, T = lax.axis_size("ep"), lax.axis_size("tp")
    local, D = moe_input.shape
    groups, experts = group_router.shape[1], expert_router.shape[1]
    per_group = experts // groups
    R = 2 * local // groups
    n, channels = mix_input.shape[0], pool_in_weight.shape[1]
    F, H, Y = D // T, expert_gate.shape[2], T // 2
    F2 = pool_out_weight.shape[1]
    steps = 4
    rows = E // steps * R
    dma = pltpu.SemaphoreType.DMA
    vmem = pl.BlockSpec(memory_space=pltpu.VMEM)
    hbm = pl.BlockSpec(memory_space=pl.ANY)
    return pl.pallas_call(
        functools.partial(block_kernel, (E, T, steps, per_group)),
        out_shape=(
            jax.ShapeDtypeStruct((n, F2), BF16),
            jax.ShapeDtypeStruct((local, F), BF16),
        ),
        in_specs=[vmem] * 7 + [hbm] * 4,
        out_specs=(vmem, vmem),
        scratch_shapes=[
            pltpu.VMEM((groups * R, D), BF16),
            pltpu.VMEM((local, D), BF16),
            pltpu.VMEM((n, D), BF16),
            pltpu.VMEM((n, channels), BF16),
            pltpu.VMEM((D, H), BF16),
            pltpu.VMEM((D, H), BF16),
            pltpu.VMEM((H, D), BF16),
            pltpu.VMEM((T, channels, F2), BF16),
            pltpu.VMEM((E * R, D), BF16),
            pltpu.VMEM((rows, H), BF16),
            pltpu.VMEM((E * R, D), BF16),
            pltpu.VMEM((steps, Y, rows, F), BF16),
            pltpu.VMEM((steps, Y, rows, F), BF16),
            pltpu.VMEM((E * R, F), BF16),
            pltpu.VMEM((E, R, F), BF16),
            pltpu.VMEM((n + 2 * HALO, channels), BF16),
            pltpu.VMEM((T, n, channels), BF16),
            dma((4,)), dma, dma((E,)), dma((E,)),
            dma((steps, Y)), dma((steps, Y)), dma((steps, Y)), dma((steps, Y)),
            dma((steps, Y)), dma((steps, Y)), dma((steps, Y)), dma((steps, Y)),
            dma((E,)), dma((E,)), dma((2,)), dma((2,)), dma((T,)), dma((T,)),
        ],
        compiler_params=pltpu.CompilerParams(
            collective_id=0, has_side_effects=True, vmem_limit_bytes=60 * 1024 * 1024
        ),
    )(
        mix_input, mix_gain[None, :], pool_in_weight, moe_input, moe_gain[None, :],
        jnp.concatenate([group_router, expert_router], axis=1), routes,
        expert_gate.reshape(D, H), expert_up.reshape(D, H), expert_down.reshape(H, D),
        pool_out_weight.reshape(T, channels, F2),
    )


def solution(mesh):
    in_specs = (
        P("ep", None), P(), P(None, "tp"), P(None, "tp"), P("ep", None), P(), P(), P(),
        P("ep", None), P("ep", None, "tp"), P("ep", None, "tp"), P("ep", "tp", None),
    )
    return jax.shard_map(
        on_device, mesh=mesh, in_specs=in_specs, out_specs=(P("ep", "tp"), P("ep", "tp")),
        check_vma=False,
    )
```
